32 devices in a mesh: grp: 2 (over y), fs: 4 (over z), tp: 4 (over x, core).
Axes of the slice: x: 2, y: 2, z: 4, core: 2. Of those that a mesh axis runs over, the one named last changes fastest.
Arguments:
- tokens: bfloat16 [8, 384, 2048], P(('grp', 'fs'), None, 'tp'), parts along dimension 0, may hold values from -16 to 16
- norm_gain: float32 [2048], P('tp'), may hold values from 0.1 to 1.9
- in_weight: bfloat16 [2048, 1024], P('fs', 'tp'), may hold values from -0.125 to 0.125
- pool_weight: bfloat16 [8, 128, 128], P('tp'), may hold values from -0.5 to 0.5
- pool_scale: float32 [1024], P('tp'), may hold values from 0.1 to 1.9
- out_weight: bfloat16 [1024, 2048], P('fs', 'tp'), may hold values from -0.1875 to 0.1875
- ffn_gain: float32 [2048], P('tp'), may hold values from 0.1 to 1.9
- gate_weight: bfloat16 [2048, 5632], P('fs', 'tp'), may hold values from -0.125 to 0.125
- up_weight: bfloat16 [2048, 5632], P('fs', 'tp'), may hold values from -0.125 to 0.125
- down_weight: bfloat16 [5632, 2048], P('tp', 'fs'), may hold values from -0.078125 to 0.078125
Outputs:
- output: bfloat16 [8, 384, 2048], P(('grp', 'fs'), None, 'tp'), parts along dimension 0
The draws below stay inside these ranges and needn't reach their ends.
There are 2 independent parts, one for each index of `grp`. The reference program is written for one: setup_inputs(seed, part) draws one part's arguments, and reference() takes and returns one part's arrays. A program takes and returns all parts, laid end to end along the dimension named above; an argument that names none is the same for every part. Nothing has to cross between parts.
All inputs are finite; a program needn't handle non-finite values.
Results may differ from the reference program's by a relative error of at most 0.009.
Values may be sent and summed in bfloat16 or wider, within the bound.
A program may use at most 64 MiB of HBM per device.

```python
import jax
import jax.numpy as jnp
from jax import lax

D = 2048
FF = 5632
GROUPS = 8
GD = 128
PW = 1024
LEN = 384
SEQS = 4
N_TP = 4


def draw_tokens(key, part):
    base_key = jax.random.fold_in(key, 11)
    noise_key, block_key, row_key = jax.random.split(base_key, 3)
    noise_draw = jax.random.normal(noise_key, (SEQS, LEN, D), jnp.float32)
    block_scale = jnp.exp(jax.random.uniform(block_key, (16,), jnp.float32, -1.4, 1.4))
    row_scale = jnp.exp(jax.random.uniform(row_key, (SEQS, LEN, 1), jnp.float32, -0.5, 0.5))
    return jnp.clip(noise_draw * jnp.repeat(block_scale, D // 16) * row_scale, -16.0, 16.0).astype(jnp.bfloat16)


def level_of(stream_key, shape, cuts, least, high):
    level, own = 1.0, jax.random.fold_in(stream_key, 6)
    for axis_at, parts in cuts:
        draws = jnp.exp(jax.random.uniform(jax.random.fold_in(own, axis_at), (parts,), jnp.float32, least / len(cuts), high / len(cuts)))
        level = level * jnp.repeat(draws, shape[axis_at] // parts).reshape([-1 if axis == axis_at else 1 for axis in range(len(shape))])
    return level


def gaussian(key, extent, scale, reach, cuts=(), held_as=jnp.bfloat16):
    entries = scale * jax.random.normal(key, extent, jnp.float32)
    if cuts:
        entries = entries * level_of(key, extent, cuts, -0.22, 0.18)
    return jnp.clip(entries, -reach, reach).astype(held_as)


def setup_inputs(seed: int = 0, part: int = 0) -> dict:
    splits = jax.random.split(jax.random.key(seed), 11)
    part_keys = jax.random.split(jax.random.fold_in(splits[10], part), 11)
    return {
        "tokens": draw_tokens(jax.random.fold_in(jax.random.fold_in(splits[10], part), 71), part),
        "norm_gain": jnp.clip(1.0 + 0.18 * jax.random.normal(splits[1], (D,), jnp.float32), 0.1, 1.9),
        "in_weight": gaussian(splits[2], (D, PW), D ** -0.5, 0.125, ((0, 4), (1, 4))),
        "pool_weight": gaussian(splits[3], (GROUPS, GD, GD), GD ** -0.5, 0.5, ((0, 4),)),
        "pool_scale": jnp.clip(1.0 + 0.18 * jax.random.normal(splits[4], (PW,), jnp.float32), 0.1, 1.9),
        "out_weight": gaussian(splits[5], (PW, D), PW ** -0.5, 0.1875, ((0, 4), (1, 4))),
        "ffn_gain": jnp.clip(1.0 + 0.18 * jax.random.normal(splits[6], (D,), jnp.float32), 0.1, 1.9),
        "gate_weight": gaussian(splits[7], (D, FF), D ** -0.5, 0.125, ((0, 4), (1, 4))),
        "up_weight": gaussian(splits[8], (D, FF), D ** -0.5, 0.125, ((0, 4), (1, 4))),
        "down_weight": gaussian(splits[9], (FF, D), FF ** -0.5, 0.078125, ((0, 4), (1, 4))),
    }


EPSILON = 0.05
HALVES = (1, 2, 4, 8)

def norm_rows(stream, gain):
    square = lax.optimization_barrier(jnp.sum(stream * stream, axis=-1, keepdims=True))
    return (stream * lax.rsqrt(square / stream.shape[-1] + EPSILON) * gain).astype(jnp.bfloat16)

def reference(tokens, norm_gain, in_weight, pool_weight, pool_scale, out_weight, ffn_gain, gate_weight, up_weight, down_weight):
    seq_count, length, width = tokens.shape
    stream = tokens.astype(jnp.float32).reshape(seq_count * length, width)
    normed = norm_rows(stream, norm_gain)
    pool_input = jnp.dot(normed, in_weight, preferred_element_type=jnp.float32).astype(jnp.bfloat16)
    pool_float = pool_input.astype(jnp.float32).reshape(seq_count, length, -1)
    running = jnp.concatenate([jnp.zeros((seq_count, 1, pool_float.shape[2]), jnp.float32), jnp.cumsum(pool_float, axis=1)], axis=1)
    position = jnp.arange(length)
    blocks = []
    for group in range(GROUPS):
        half_width = HALVES[group % 4]
        lower_index = jnp.clip(position - half_width, 0, length)
        upper_index = jnp.clip(position + half_width, 0, length)
        group_sums = running[:, :, group * GD:(group + 1) * GD]
        counts = (upper_index - lower_index).astype(jnp.float32)
        window_mean = (group_sums[:, upper_index] - group_sums[:, lower_index]) / counts[:, None]
        blocks.append(window_mean - pool_float[:, :, group * GD:(group + 1) * GD])
    deviation = jnp.stack(blocks, axis=2).astype(jnp.bfloat16)
    mapped = jnp.einsum('slgc,gcd->slgd', deviation.astype(jnp.float32), pool_weight.astype(jnp.float32))
    pooled = (mapped.reshape(seq_count * length, GROUPS * GD) * pool_scale).astype(jnp.bfloat16)
    mixed = stream + jnp.dot(pooled, out_weight, preferred_element_type=jnp.float32)
    normed_two = norm_rows(mixed, ffn_gain)
    gate_out = jnp.dot(normed_two, gate_weight, preferred_element_type=jnp.float32)
    up_out = jnp.dot(normed_two, up_weight, preferred_element_type=jnp.float32)
    hidden = (jax.nn.silu(gate_out) * up_out).astype(jnp.bfloat16)
    block_size = FF // N_TP
    summed = jnp.zeros_like(mixed)
    for block_index in range(N_TP):
        lower_unit = block_index * block_size
        partial_value = jnp.dot(hidden[:, lower_unit:lower_unit + block_size], down_weight[lower_unit:lower_unit + block_size], preferred_element_type=jnp.float32).astype(jnp.bfloat16)
        summed = summed + partial_value.astype(jnp.float32)
    return (mixed + summed).astype(jnp.bfloat16).reshape(seq_count, length, width)
```

```python
import functools

import jax
import jax.numpy as jnp
from jax import lax
from jax.experimental import pallas as pl
from jax.experimental.pallas import tpu as pltpu
from jax.sharding import PartitionSpec as P

D = 2048
GD = 128


EPSILON = 0.05
HALVES = (1, 2, 4, 8)


def local(
    tokens,
    norm_gain,
    in_weight,
    pool_weight,
    pool_scale,
    out_weight,
    ffn_gain,
    gate_weight,
    up_weight,
    down_weight,
):
    seq_local, length, feat_local = tokens.shape
    stream = tokens.astype(jnp.float32)
    first_square = lax.psum(jnp.sum(stream * stream, axis=-1), "tp")
    normed = (stream * lax.rsqrt(first_square[..., None] / D + EPSILON) * norm_gain).astype(
        jnp.bfloat16
    )
    in_full = lax.all_gather(in_weight, "fs", axis=0, tiled=True)
    channels = in_full.shape[1]
    weight_rows = in_full
    pool_input = jnp.einsum(
        "slk,kc->slc",
        lax.all_gather(normed, "tp", axis=2, tiled=True),
        weight_rows,
        preferred_element_type=jnp.float32,
    ).astype(jnp.bfloat16)
    pool_float = pool_input.astype(jnp.float32)
    group_local = pool_weight.shape[0]
    group_ids = lax.axis_index("tp") * group_local + jnp.arange(channels) // GD
    selector = group_ids % 4
    running = jnp.concatenate(
        [jnp.zeros((seq_local, 1, channels), jnp.float32), jnp.cumsum(pool_float, axis=1)], axis=1
    )
    position = jnp.arange(length)
    window_mean = jnp.zeros_like(pool_float)
    for window_index, half_width in enumerate(HALVES):
        upper_sum = jnp.concatenate(
            [running[:, half_width:], jnp.repeat(running[:, -1:], half_width, axis=1)], axis=1
        )[:, :length]
        lower_sum = jnp.concatenate(
            [
                jnp.zeros((seq_local, half_width, channels), jnp.float32),
                running[:, : length + 1 - half_width],
            ],
            axis=1,
        )[:, :length]
        counts = (
            jnp.minimum(position + half_width, length) - jnp.maximum(position - half_width, 0)
        ).astype(jnp.float32)
        window_mean = jnp.where(
            selector == window_index, (upper_sum - lower_sum) / counts[:, None], window_mean
        )
    deviation = (window_mean - pool_float).astype(jnp.bfloat16)
    grouped = deviation.reshape(seq_local, length, group_local, GD)
    mapped = jnp.einsum("slgc,gcd->slgd", grouped, pool_weight, preferred_element_type=jnp.float32)
    pooled = (mapped.reshape(seq_local, length, channels) * pool_scale).astype(jnp.bfloat16)
    out_full = lax.all_gather(out_weight, "fs", axis=0, tiled=True)
    weight_rows = out_full
    mixed = stream + jnp.einsum(
        "jut,tx->jux",
        lax.all_gather(pooled, "tp", axis=2, tiled=True),
        weight_rows,
        preferred_element_type=jnp.float32,
    )
    second_square = lax.psum(jnp.sum(mixed * mixed, axis=-1), "tp")
    normed_two = (mixed * lax.rsqrt(second_square[..., None] / D + EPSILON) * ffn_gain).astype(
        jnp.bfloat16
    )
    features_full = lax.all_gather(normed_two, "tp", axis=2, tiled=True)
    gate_sum = jnp.einsum(
        "slk,kf->slf",
        features_full,
        lax.all_gather(gate_weight, "fs", axis=0, tiled=True),
        preferred_element_type=jnp.float32,
    )
    up_sum = jnp.einsum(
        "slk,kf->slf",
        features_full,
        lax.all_gather(up_weight, "fs", axis=0, tiled=True),
        preferred_element_type=jnp.float32,
    )
    hidden = (jax.nn.silu(gate_sum) * up_sum).astype(jnp.bfloat16)
    partial_value = jnp.einsum(
        "hor,rn->hon",
        hidden,
        lax.all_gather(down_weight, "fs", axis=1, tiled=True),
        preferred_element_type=jnp.float32,
    )
    summed = lax.psum_scatter(
        partial_value.astype(jnp.bfloat16), "tp", scatter_dimension=2, tiled=True
    ).astype(jnp.float32)
    return (mixed + summed).astype(jnp.bfloat16)


SPLITS = (1, 1, 2, 2, 4)
W_IN, W_OUT, W_GATE, W_UP, W_DOWN = range(5)
FIRST = tuple(sum(SPLITS[:k]) for k in range(5))
E_TOK, E_GAIN, E_POOL, E_SQ, E_X2, E_RS = range(6)
MESH = pl.DeviceIdType.MESH


def kernel(
    n_fs,
    n_tp,
    tokens,
    gain1,
    pool_w,
    scale,
    gain2,
    w_in,
    w_out,
    w_gate,
    w_up,
    w_down,
    out,
    b_in,
    b_out,
    b_gate,
    b_up,
    b_down,
    tok,
    gain_all,
    pooled,
    sq,
    x2,
    mixed,
    gate_acc,
    hidden,
    part,
    rs,
    stage,
    z_recv,
    y_recv,
    r_send,
    l_send,
    y_send,
    own_sem,
    e_send,
    e_recv,
):
    g, i, j = lax.axis_index("grp"), lax.axis_index("fs"), lax.axis_index("tp")
    length, feat = tokens.shape
    bufs = (b_in, b_out, b_gate, b_up, b_down)
    srcs = (w_in, w_out, w_gate, w_up, w_down)
    has_left, has_right = i > 0, i < n_fs - 1

    barrier = pltpu.get_barrier_semaphore()

    def greet(device):
        pl.semaphore_signal(barrier, inc=1, device_id=device, device_id_type=MESH)

    pl.when(has_left)(lambda: greet({"fs": i - 1}))
    pl.when(has_right)(lambda: greet({"fs": i + 1}))
    greet({"grp": 1 - g})
    for o in range(1, n_tp):
        greet({"tp": lax.rem(j + o, n_tp)})
    pl.semaphore_wait(barrier, n_tp + jnp.minimum(i, 1) + jnp.minimum(n_fs - 1 - i, 1))

    def rows(k):
        return srcs[k].shape[0]

    def slot(k, s, half, q):
        step = rows(k) // 2 // SPLITS[k]
        off = pl.multiple_of(s * rows(k) + half * (rows(k) // 2) + q * step, 16)
        return bufs[k].at[pl.ds(off, step)]

    def own_rows(k, q):
        step = rows(k) // 2 // SPLITS[k]
        return srcs[k].at[pl.ds(pl.multiple_of(g * (rows(k) // 2) + q * step, 16), step)]

    def z_copy(k, q, s, right, own):
        item = FIRST[k] + q
        return pltpu.make_async_remote_copy(
            src_ref=own_rows(k, q) if own else slot(k, s, g, q),
            dst_ref=slot(k, s, g, q),
            send_sem=(r_send if right else l_send).at[item, s],
            recv_sem=z_recv.at[item, s],
            device_id={"fs": i + 1 if right else i - 1},
            device_id_type=MESH,
        )

    def y_copy(k, q, s, half):
        item = FIRST[k] + q
        return pltpu.make_async_remote_copy(
            src_ref=slot(k, s, half, q),
            dst_ref=slot(k, s, half, q),
            send_sem=y_send.at[item, s],
            recv_sem=y_recv.at[item, s],
            device_id={"grp": 1 - g},
            device_id_type=MESH,
        )

    def send_own(k):
        for q in range(SPLITS[k]):
            pl.when(has_right)(lambda q=q: z_copy(k, q, i, True, True).start())
            pl.when(has_left)(lambda q=q: z_copy(k, q, i, False, True).start())

    def serve(k, d, q):
        @pl.when(i - d >= 0)
        def _():
            s = i - d
            z_copy(k, q, s, True, False).wait_recv()
            pl.when(has_right)(lambda: z_copy(k, q, s, True, False).start())
            y_copy(k, q, s, g).start()

        @pl.when(i + d < n_fs)
        def _():
            s = i + d
            z_copy(k, q, s, False, False).wait_recv()
            pl.when(has_left)(lambda: z_copy(k, q, s, False, False).start())
            y_copy(k, q, s, g).start()

    def serve_all(k, d):
        for q in range(SPLITS[k]):
            serve(k, d, q)

    def each(d, f):
        pl.when(i - d >= 0)(lambda: f(i - d))
        pl.when(i + d < n_fs)(lambda: f(i + d))

    def wait_y(k, s):
        for q in range(SPLITS[k]):
            y_copy(k, q, s, 1 - g).wait_recv()

    def own_copy(k):
        off = pl.multiple_of(i * rows(k), 16)
        return pltpu.make_async_copy(srcs[k], bufs[k].at[pl.ds(off, rows(k))], own_sem.at[k])

    def arrived(k):
        own_copy(k).wait()
        for d in range(1, n_fs):
            each(d, lambda s: wait_y(k, s))

    def cols(ref, t, width):
        return ref.at[:, pl.ds(pl.multiple_of(t * width, 128), width)]

    def e_copy(e, o, src, dst):
        return pltpu.make_async_remote_copy(
            src_ref=src,
            dst_ref=dst(j),
            send_sem=e_send.at[e, o],
            recv_sem=e_recv.at[e, j],
            device_id={"tp": lax.rem(j + o, n_tp)},
            device_id_type=MESH,
        )

    def share(e, src, dst):
        for o in range(1, n_tp):
            e_copy(e, o, src, dst).start()

    def take(e, src, dst):
        for o in range(1, n_tp):
            p = lax.rem(j + o, n_tp)
            pltpu.make_async_remote_copy(
                src_ref=src,
                dst_ref=dst(p),
                send_sem=e_send.at[e, o],
                recv_sem=e_recv.at[e, p],
                device_id={"tp": p},
                device_id_type=MESH,
            ).wait_recv()

    channels = w_in.shape[1]
    tok_at = lambda t: cols(tok, t, feat)
    gain_at = lambda t: cols(gain_all, t, feat)
    pool_at = lambda t: cols(pooled, t, channels)
    sq_at = lambda t: sq.at[t]
    x2_at = lambda t: cols(x2, t, feat)

    send_own(W_IN)
    send_own(W_OUT)
    share(E_TOK, tokens, tok_at)
    share(E_GAIN, gain1, gain_at)
    for k in range(5):
        own_copy(k).start()
    cols(tok, j, feat)[...] = tokens[...]
    cols(gain_all, j, feat)[...] = gain1[...]
    for d in range(1, n_fs):
        serve_all(W_IN, d)
        serve_all(W_OUT, d)
    send_own(W_GATE)
    send_own(W_UP)

    take(E_TOK, tokens, tok_at)
    take(E_GAIN, gain1, gain_at)
    width = tok.shape[1]
    block = 32
    @pl.loop(0, length // block)
    def _(r):
        at = pl.ds(pl.multiple_of(r * block, block), block)
        x = tok[at, :].astype(jnp.float32)
        square = jnp.sum(x * x, axis=-1, keepdims=True)
        x2[at, :] = (x * lax.rsqrt(square / width + EPSILON) * gain_all[0:1, :]).astype(
            jnp.bfloat16
        )

    arrived(W_IN)
    pool_in = jnp.dot(x2[...], b_in[...], preferred_element_type=jnp.float32).astype(jnp.bfloat16)
    group_local = pool_w.shape[0]
    row = lax.broadcasted_iota(jnp.int32, (length, length), 0)
    col = lax.broadcasted_iota(jnp.int32, (length, length), 1)
    at_row = lax.broadcasted_iota(jnp.int32, (length, 128), 0)
    for k in range(group_local):
        level = lax.rem(j * group_local + k, len(HALVES))
        half = jnp.int32(HALVES[0])
        for index, value in enumerate(HALVES):
            half = jnp.where(level == index, jnp.int32(value), half)
        inside = (col >= row - half) & (col < row + half)
        band = jnp.where(inside, 1.0, 0.0).astype(jnp.bfloat16)
        count = jnp.minimum(at_row + half, length) - jnp.maximum(at_row - half, 0)
        piece = pool_in[:, k * GD : (k + 1) * GD]
        total = jnp.dot(band, piece, preferred_element_type=jnp.float32)
        deviation = total / count[:, :1].astype(jnp.float32) - piece.astype(jnp.float32)
        mapped = jnp.dot(
            deviation.astype(jnp.bfloat16), pool_w[k], preferred_element_type=jnp.float32
        )
        stage[:, k * GD : (k + 1) * GD] = (
            mapped * scale[0:1, k * GD : (k + 1) * GD]
        ).astype(jnp.bfloat16)
    own_pool = stage.at[:, pl.ds(0, channels)]
    cols(pooled, j, channels)[...] = own_pool[...]
    share(E_POOL, own_pool, pool_at)
    serve_all(W_GATE, 1)
    send_own(W_DOWN)
    arrived(W_OUT)
    take(E_POOL, own_pool, pool_at)
    mixed[...] = tokens[...].astype(jnp.float32) + jnp.dot(
        pooled[...], b_out[...], preferred_element_type=jnp.float32
    )
    partial_sq = jnp.zeros((length, 128), jnp.float32)
    for c in range(feat // 128):
        m = mixed[:, c * 128 : (c + 1) * 128]
        partial_sq = partial_sq + m * m
    own_sq = sq.at[n_tp]
    own_sq[...] = partial_sq
    share(E_SQ, own_sq, sq_at)
    take(E_SQ, own_sq, sq_at)
    total_sq = sq[n_tp]
    for o in range(1, n_tp):
        total_sq = total_sq + sq[lax.rem(j + o, n_tp)]
    second = jnp.sum(total_sq, axis=-1, keepdims=True)
    own_x2 = stage.at[:, pl.ds(channels, feat)]
    own_x2[...] = (mixed[...] * lax.rsqrt(second / width + EPSILON) * gain2[0:1, :]).astype(
        jnp.bfloat16
    )
    x2_full = tok
    cols(x2_full, j, feat)[...] = own_x2[...]
    x2_at = lambda t: cols(x2_full, t, feat)
    share(E_X2, own_x2, x2_at)

    for d in range(2, n_fs):
        serve_all(W_GATE, d)
    take(E_X2, own_x2, x2_at)
    serve_all(W_UP, 1)
    arrived(W_GATE)

    def project(b, acc, at):
        depth = 512 if width % 512 == 0 else 128
        acc[...] = jnp.zeros_like(acc)

        @pl.loop(0, width // depth)
        def _(c):
            k_at = pl.ds(pl.multiple_of(c * depth, depth), depth)
            acc[...] += jnp.dot(at[:, k_at], b[k_at, :], preferred_element_type=jnp.float32)

    project(b_gate, gate_acc, x2_full)
    for d in range(2, n_fs):
        serve_all(W_UP, d)
    serve_all(W_DOWN, 1)
    arrived(W_UP)
    up_chunk = 64

    @pl.loop(0, length // up_chunk)
    def _(r):
        at = pl.ds(pl.multiple_of(r * up_chunk, up_chunk), up_chunk)
        up = jnp.dot(x2_full[at, :], b_up[...], preferred_element_type=jnp.float32)
        gate = gate_acc[at, :]
        hidden[at, :] = (gate / (1.0 + jnp.exp(-gate)) * up).astype(jnp.bfloat16)

    def rs_copy(s):
        return pltpu.make_async_remote_copy(
            src_ref=part.at[s],
            dst_ref=rs.at[j],
            send_sem=e_send.at[E_RS, s],
            recv_sem=e_recv.at[E_RS, j],
            device_id={"tp": s},
            device_id_type=MESH,
        )

    def down(s):
        at = pl.ds(pl.multiple_of(s * rows(W_DOWN), 16), rows(W_DOWN))
        part[s] = jnp.dot(
            hidden[...], b_down[at, :], preferred_element_type=jnp.float32
        ).astype(jnp.bfloat16)
        pl.when(s != j)(lambda: rs_copy(s).start())

    own_copy(W_DOWN).wait()
    down(i)
    for d in range(1, n_fs):
        if d > 1:
            serve_all(W_DOWN, d)

        def finish(s):
            wait_y(W_DOWN, s)
            down(s)

        each(d, finish)

    for o in range(1, n_tp):
        p = lax.rem(j + o, n_tp)
        pltpu.make_async_remote_copy(
            src_ref=part.at[p],
            dst_ref=rs.at[p],
            send_sem=e_send.at[E_RS, p],
            recv_sem=e_recv.at[E_RS, p],
            device_id={"tp": p},
            device_id_type=MESH,
        ).wait_recv()
    summed = part[j].astype(jnp.float32)
    for o in range(1, n_tp):
        summed = summed + rs[lax.rem(j + o, n_tp)].astype(jnp.float32)
    out[...] = (mixed[...] + summed).astype(jnp.bfloat16)

    for k in range(5):
        for q in range(SPLITS[k]):
            pl.when(has_right)(lambda k=k, q=q: z_copy(k, q, i, True, True).wait_send())
            pl.when(has_left)(lambda k=k, q=q: z_copy(k, q, i, False, True).wait_send())
            for d in range(1, n_fs):

                @pl.when(i - d >= 0)
                def _(k=k, q=q, d=d):
                    pl.when(has_right)(lambda: z_copy(k, q, i - d, True, False).wait_send())
                    y_copy(k, q, i - d, g).wait_send()

                @pl.when(i + d < n_fs)
                def _(k=k, q=q, d=d):
                    pl.when(has_left)(lambda: z_copy(k, q, i + d, False, False).wait_send())
                    y_copy(k, q, i + d, g).wait_send()

    for o in range(1, n_tp):
        e_copy(E_TOK, o, tokens, tok_at).wait_send()
        e_copy(E_GAIN, o, gain1, gain_at).wait_send()
        e_copy(E_POOL, o, own_pool, pool_at).wait_send()
        e_copy(E_SQ, o, own_sq, sq_at).wait_send()
        e_copy(E_X2, o, own_x2, x2_at).wait_send()
        rs_copy(lax.rem(j + o, n_tp)).wait_send()


def fused(
    n_fs,
    n_tp,
    tokens,
    norm_gain,
    in_weight,
    pool_weight,
    pool_scale,
    out_weight,
    ffn_gain,
    gate_weight,
    up_weight,
    down_weight,
):
    _, length, feat = tokens.shape
    channels, units = in_weight.shape[1], gate_weight.shape[1]
    weights = (in_weight, out_weight, gate_weight, up_weight, down_weight)
    wide = lambda v: jnp.broadcast_to(v, (8, v.shape[0]))
    vmem = pl.BlockSpec(memory_space=pltpu.VMEM)
    hbm = pl.BlockSpec(memory_space=pl.ANY)
    items = sum(SPLITS)
    bf16, f32 = jnp.bfloat16, jnp.float32
    sems = pltpu.SemaphoreType.DMA
    return pl.pallas_call(
        functools.partial(kernel, n_fs, n_tp),
        out_shape=jax.ShapeDtypeStruct((length, feat), bf16),
        in_specs=[vmem] * 5 + [hbm] * 5,
        out_specs=vmem,
        scratch_shapes=[pltpu.VMEM((n_fs * w.shape[0], w.shape[1]), bf16) for w in weights]
        + [
            pltpu.VMEM((length, n_tp * feat), bf16),
            pltpu.VMEM((8, n_tp * feat), f32),
            pltpu.VMEM((length, n_tp * channels), bf16),
            pltpu.VMEM((n_tp + 1, length, 128), f32),
            pltpu.VMEM((length, n_tp * feat), bf16),
            pltpu.VMEM((length, feat), f32),
            pltpu.VMEM((length, units), f32),
            pltpu.VMEM((length, units), bf16),
            pltpu.VMEM((n_tp, length, feat), bf16),
            pltpu.VMEM((n_tp, length, feat), bf16),
            pltpu.VMEM((length, channels + feat), bf16),
        ]
        + [sems((items, n_fs))] * 5
        + [sems((5,)), sems((6, n_tp)), sems((6, n_tp))],
        compiler_params=pltpu.CompilerParams(
            collective_id=0, has_side_effects=True, vmem_limit_bytes=56 * 1024 * 1024
        ),
    )(
        tokens[0],
        wide(norm_gain),
        pool_weight,
        wide(pool_scale),
        wide(ffn_gain),
        *weights,
    )[None]


def solution(mesh):
    n_grp, n_fs, n_tp = mesh.shape["grp"], mesh.shape["fs"], mesh.shape["tp"]
    body = functools.partial(fused, n_fs, n_tp) if n_grp == 2 and n_fs == n_tp <= 8 else local
    return jax.shard_map(
        body,
        mesh=mesh,
        in_specs=(
            P(("grp", "fs"), None, "tp"),
            P("tp"),
            P("fs", "tp"),
            P("tp", None, None),
            P("tp"),
            P("fs", "tp"),
            P("tp"),
            P("fs", "tp"),
            P("fs", "tp"),
            P("tp", "fs"),
        ),
        out_specs=P(("grp", "fs"), None, "tp"),
        check_vma=False,
    )
```

```python
import functools

import jax
import jax.numpy as jnp
from jax import lax
from jax.experimental import pallas as pl
from jax.experimental.pallas import tpu as pltpu
from jax.sharding import PartitionSpec as P

D = 2048
GD = 128


EPSILON = 0.05
HALVES = (1, 2, 4, 8)


def local(
    tokens,
    norm_gain,
    in_weight,
    pool_weight,
    pool_scale,
    out_weight,
    ffn_gain,
    gate_weight,
    up_weight,
    down_weight,
):
    seq_local, length, feat_local = tokens.shape
    stream = tokens.astype(jnp.float32)
    first_square = lax.psum(jnp.sum(stream * stream, axis=-1), "tp")
    normed = (stream * lax.rsqrt(first_square[..., None] / D + EPSILON) * norm_gain).astype(
        jnp.bfloat16
    )
    in_full = lax.all_gather(in_weight, "fs", axis=0, tiled=True)
    channels = in_full.shape[1]
    weight_rows = in_full
    pool_input = jnp.einsum(
        "slk,kc->slc",
        lax.all_gather(normed, "tp", axis=2, tiled=True),
        weight_rows,
        preferred_element_type=jnp.float32,
    ).astype(jnp.bfloat16)
    pool_float = pool_input.astype(jnp.float32)
    group_local = pool_weight.shape[0]
    group_ids = lax.axis_index("tp") * group_local + jnp.arange(channels) // GD
    selector = group_ids % 4
    running = jnp.concatenate(
        [jnp.zeros((seq_local, 1, channels), jnp.float32), jnp.cumsum(pool_float, axis=1)], axis=1
    )
    position = jnp.arange(length)
    window_mean = jnp.zeros_like(pool_float)
    for window_index, half_width in enumerate(HALVES):
        upper_sum = jnp.concatenate(
            [running[:, half_width:], jnp.repeat(running[:, -1:], half_width, axis=1)], axis=1
        )[:, :length]
        lower_sum = jnp.concatenate(
            [
                jnp.zeros((seq_local, half_width, channels), jnp.float32),
                running[:, : length + 1 - half_width],
            ],
            axis=1,
        )[:, :length]
        counts = (
            jnp.minimum(position + half_width, length) - jnp.maximum(position - half_width, 0)
        ).astype(jnp.float32)
        window_mean = jnp.where(
            selector == window_index, (upper_sum - lower_sum) / counts[:, None], window_mean
        )
    deviation = (window_mean - pool_float).astype(jnp.bfloat16)
    grouped = deviation.reshape(seq_local, length, group_local, GD)
    mapped = jnp.einsum("slgc,gcd->slgd", grouped, pool_weight, preferred_element_type=jnp.float32)
    pooled = (mapped.reshape(seq_local, length, channels) * pool_scale).astype(jnp.bfloat16)
    out_full = lax.all_gather(out_weight, "fs", axis=0, tiled=True)
    weight_rows = out_full
    mixed = stream + jnp.einsum(
        "jut,tx->jux",
        lax.all_gather(pooled, "tp", axis=2, tiled=True),
        weight_rows,
        preferred_element_type=jnp.float32,
    )
    second_square = lax.psum(jnp.sum(mixed * mixed, axis=-1), "tp")
    normed_two = (mixed * lax.rsqrt(second_square[..., None] / D + EPSILON) * ffn_gain).astype(
        jnp.bfloat16
    )
    features_full = lax.all_gather(normed_two, "tp", axis=2, tiled=True)
    gate_sum = jnp.einsum(
        "slk,kf->slf",
        features_full,
        lax.all_gather(gate_weight, "fs", axis=0, tiled=True),
        preferred_element_type=jnp.float32,
    )
    up_sum = jnp.einsum(
        "slk,kf->slf",
        features_full,
        lax.all_gather(up_weight, "fs", axis=0, tiled=True),
        preferred_element_type=jnp.float32,
    )
    hidden = (jax.nn.silu(gate_sum) * up_sum).astype(jnp.bfloat16)
    partial_value = jnp.einsum(
        "hor,rn->hon",
        hidden,
        lax.all_gather(down_weight, "fs", axis=1, tiled=True),
        preferred_element_type=jnp.float32,
    )
    summed = lax.psum_scatter(
        partial_value.astype(jnp.bfloat16), "tp", scatter_dimension=2, tiled=True
    ).astype(jnp.float32)
    return (mixed + summed).astype(jnp.bfloat16)


SPLITS = (1, 1, 4, 2, 4)
W_IN, W_OUT, W_GATE, W_UP, W_DOWN = range(5)
FIRST = tuple(sum(SPLITS[:k]) for k in range(5))
E_TOK, E_GAIN, E_POOL, E_SQ, E_X2, E_RS = range(6)
MESH = pl.DeviceIdType.MESH


def kernel(
    n_fs,
    n_tp,
    tokens,
    gain1,
    pool_w,
    scale,
    gain2,
    w_in,
    w_out,
    w_gate,
    w_up,
    w_down,
    out,
    b_in,
    b_out,
    b_gate,
    b_up,
    b_down,
    tok,
    gain_all,
    pooled,
    sq,
    x2,
    mixed,
    gate_acc,
    hidden,
    part,
    rs,
    stage,
    z_recv,
    y_recv,
    r_send,
    l_send,
    y_send,
    own_sem,
    e_send,
    e_recv,
):
    g, i, j = lax.axis_index("grp"), lax.axis_index("fs"), lax.axis_index("tp")
    length, feat = tokens.shape
    bufs = (b_in, b_out, b_gate, b_up, b_down)
    srcs = (w_in, w_out, w_gate, w_up, w_down)
    has_left, has_right = i > 0, i < n_fs - 1

    barrier = pltpu.get_barrier_semaphore()

    def greet(device):
        pl.semaphore_signal(barrier, inc=1, device_id=device, device_id_type=MESH)

    pl.when(has_left)(lambda: greet({"fs": i - 1}))
    pl.when(has_right)(lambda: greet({"fs": i + 1}))
    greet({"grp": 1 - g})
    for o in range(1, n_tp):
        greet({"tp": lax.rem(j + o, n_tp)})
    pl.semaphore_wait(barrier, n_tp + jnp.minimum(i, 1) + jnp.minimum(n_fs - 1 - i, 1))

    def rows(k):
        return srcs[k].shape[0]

    def slot(k, s, half, q):
        step = rows(k) // 2 // SPLITS[k]
        off = pl.multiple_of(s * rows(k) + half * (rows(k) // 2) + q * step, 16)
        return bufs[k].at[pl.ds(off, step)]

    def own_rows(k, q):
        step = rows(k) // 2 // SPLITS[k]
        return srcs[k].at[pl.ds(pl.multiple_of(g * (rows(k) // 2) + q * step, 16), step)]

    def z_copy(k, q, s, right, own):
        item = FIRST[k] + q
        return pltpu.make_async_remote_copy(
            src_ref=own_rows(k, q) if own else slot(k, s, g, q),
            dst_ref=slot(k, s, g, q),
            send_sem=(r_send if right else l_send).at[item, s],
            recv_sem=z_recv.at[item, s],
            device_id={"fs": i + 1 if right else i - 1},
            device_id_type=MESH,
        )

    def y_copy(k, q, s, half):
        item = FIRST[k] + q
        return pltpu.make_async_remote_copy(
            src_ref=slot(k, s, half, q),
            dst_ref=slot(k, s, half, q),
            send_sem=y_send.at[item, s],
            recv_sem=y_recv.at[item, s],
            device_id={"grp": 1 - g},
            device_id_type=MESH,
        )

    def send_own(k, first=0, last=None):
        for q in range(SPLITS[k])[first:last]:
            pl.when(has_right)(lambda q=q: z_copy(k, q, i, True, True).start())
            pl.when(has_left)(lambda q=q: z_copy(k, q, i, False, True).start())

    def serve(k, d, q):
        @pl.when(i - d >= 0)
        def _():
            s = i - d
            z_copy(k, q, s, True, False).wait_recv()
            pl.when(has_right)(lambda: z_copy(k, q, s, True, False).start())
            y_copy(k, q, s, g).start()

        @pl.when(i + d < n_fs)
        def _():
            s = i + d
            z_copy(k, q, s, False, False).wait_recv()
            pl.when(has_left)(lambda: z_copy(k, q, s, False, False).start())
            y_copy(k, q, s, g).start()

    def serve_all(k, d, first=0, last=None):
        for q in range(SPLITS[k])[first:last]:
            serve(k, d, q)

    def each(d, f):
        pl.when(i - d >= 0)(lambda: f(i - d))
        pl.when(i + d < n_fs)(lambda: f(i + d))

    def wait_y(k, s):
        for q in range(SPLITS[k]):
            y_copy(k, q, s, 1 - g).wait_recv()

    def own_copy(k):
        off = pl.multiple_of(i * rows(k), 16)
        return pltpu.make_async_copy(srcs[k], bufs[k].at[pl.ds(off, rows(k))], own_sem.at[k])

    def arrived(k):
        own_copy(k).wait()
        for d in range(1, n_fs):
            each(d, lambda s: wait_y(k, s))

    def cols(ref, t, width):
        return ref.at[:, pl.ds(pl.multiple_of(t * width, 128), width)]

    def e_copy(e, o, src, dst):
        return pltpu.make_async_remote_copy(
            src_ref=src,
            dst_ref=dst(j),
            send_sem=e_send.at[e, o],
            recv_sem=e_recv.at[e, j],
            device_id={"tp": lax.rem(j + o, n_tp)},
            device_id_type=MESH,
        )

    def share(e, src, dst):
        for o in range(1, n_tp):
            e_copy(e, o, src, dst).start()

    def take(e, src, dst):
        for o in range(1, n_tp):
            p = lax.rem(j + o, n_tp)
            pltpu.make_async_remote_copy(
                src_ref=src,
                dst_ref=dst(p),
                send_sem=e_send.at[e, o],
                recv_sem=e_recv.at[e, p],
                device_id={"tp": p},
                device_id_type=MESH,
            ).wait_recv()

    channels = w_in.shape[1]
    tok_at = lambda t: cols(tok, t, feat)
    gain_at = lambda t: cols(gain_all, t, feat)
    pool_at = lambda t: cols(pooled, t, channels)
    sq_at = lambda t: sq.at[t]
    x2_at = lambda t: cols(x2, t, feat)

    send_own(W_IN)
    send_own(W_OUT)
    gate_half = SPLITS[W_GATE] // 2
    send_own(W_GATE, 0, gate_half)
    share(E_TOK, tokens, tok_at)
    share(E_GAIN, gain1, gain_at)
    for k in range(5):
        own_copy(k).start()
    cols(tok, j, feat)[...] = tokens[...]
    cols(gain_all, j, feat)[...] = gain1[...]
    for d in range(1, n_fs):
        serve_all(W_IN, d)
        serve_all(W_OUT, d)
        if d == 1:
            send_own(W_GATE, gate_half)
            serve_all(W_GATE, 1, 0, gate_half)
    send_own(W_UP)
    send_own(W_DOWN)

    take(E_TOK, tokens, tok_at)
    take(E_GAIN, gain1, gain_at)
    width = tok.shape[1]
    block = 32
    @pl.loop(0, length // block)
    def _(r):
        at = pl.ds(pl.multiple_of(r * block, block), block)
        x = tok[at, :].astype(jnp.float32)
        square = jnp.sum(x * x, axis=-1, keepdims=True)
        x2[at, :] = (x * lax.rsqrt(square / width + EPSILON) * gain_all[0:1, :]).astype(
            jnp.bfloat16
        )

    serve_all(W_GATE, 1, gate_half)
    arrived(W_IN)
    pool_in = jnp.dot(x2[...], b_in[...], preferred_element_type=jnp.float32).astype(jnp.bfloat16)
    group_local = pool_w.shape[0]
    row = lax.broadcasted_iota(jnp.int32, (length, length), 0)
    col = lax.broadcasted_iota(jnp.int32, (length, length), 1)
    at_row = lax.broadcasted_iota(jnp.int32, (length, 128), 0)
    for k in range(group_local):
        level = lax.rem(j * group_local + k, len(HALVES))
        half = jnp.int32(HALVES[0])
        for index, value in enumerate(HALVES):
            half = jnp.where(level == index, jnp.int32(value), half)
        inside = (col >= row - half) & (col < row + half)
        band = jnp.where(inside, 1.0, 0.0).astype(jnp.bfloat16)
        count = jnp.minimum(at_row + half, length) - jnp.maximum(at_row - half, 0)
        piece = pool_in[:, k * GD : (k + 1) * GD]
        total = jnp.dot(band, piece, preferred_element_type=jnp.float32)
        deviation = total / count[:, :1].astype(jnp.float32) - piece.astype(jnp.float32)
        mapped = jnp.dot(
            deviation.astype(jnp.bfloat16), pool_w[k], preferred_element_type=jnp.float32
        )
        stage[:, k * GD : (k + 1) * GD] = (
            mapped * scale[0:1, k * GD : (k + 1) * GD]
        ).astype(jnp.bfloat16)
    own_pool = stage.at[:, pl.ds(0, channels)]
    cols(pooled, j, channels)[...] = own_pool[...]
    share(E_POOL, own_pool, pool_at)
    serve_all(W_UP, 1, 0, 1)
    arrived(W_OUT)
    take(E_POOL, own_pool, pool_at)
    mixed[...] = tokens[...].astype(jnp.float32) + jnp.dot(
        pooled[...], b_out[...], preferred_element_type=jnp.float32
    )
    partial_sq = jnp.zeros((length, 128), jnp.float32)
    for c in range(feat // 128):
        m = mixed[:, c * 128 : (c + 1) * 128]
        partial_sq = partial_sq + m * m
    own_sq = sq.at[n_tp]
    own_sq[...] = partial_sq
    share(E_SQ, own_sq, sq_at)
    serve_all(W_UP, 1, 1)
    take(E_SQ, own_sq, sq_at)
    total_sq = sq[n_tp]
    for o in range(1, n_tp):
        total_sq = total_sq + sq[lax.rem(j + o, n_tp)]
    second = jnp.sum(total_sq, axis=-1, keepdims=True)
    own_x2 = stage.at[:, pl.ds(channels, feat)]
    own_x2[...] = (mixed[...] * lax.rsqrt(second / width + EPSILON) * gain2[0:1, :]).astype(
        jnp.bfloat16
    )
    x2_full = tok
    cols(x2_full, j, feat)[...] = own_x2[...]
    x2_at = lambda t: cols(x2_full, t, feat)
    share(E_X2, own_x2, x2_at)

    serve_all(W_DOWN, 1)
    take(E_X2, own_x2, x2_at)
    for d in range(2, n_fs):
        serve_all(W_GATE, d)
        if d < n_fs - 1:
            serve_all(W_UP, d)
            serve_all(W_DOWN, d)
    serve_all(W_UP, n_fs - 1, 0, 1)
    arrived(W_GATE)

    def project(b, acc, at):
        depth = 512 if width % 512 == 0 else 128
        acc[...] = jnp.zeros_like(acc)

        @pl.loop(0, width // depth)
        def _(c):
            k_at = pl.ds(pl.multiple_of(c * depth, depth), depth)
            acc[...] += jnp.dot(at[:, k_at], b[k_at, :], preferred_element_type=jnp.float32)

    project(b_gate, gate_acc, x2_full)
    serve_all(W_UP, n_fs - 1, 1)
    down_half = SPLITS[W_DOWN] // 2
    serve_all(W_DOWN, n_fs - 1, 0, down_half)
    arrived(W_UP)
    up_chunk = 128

    @pl.loop(0, length // up_chunk)
    def _(r):
        at = pl.ds(pl.multiple_of(r * up_chunk, up_chunk), up_chunk)
        up = jnp.dot(x2_full[at, :], b_up[...], preferred_element_type=jnp.float32)
        gate = gate_acc[at, :]
        hidden[at, :] = (gate / (1.0 + jnp.exp(-gate)) * up).astype(jnp.bfloat16)

    def rs_copy(s):
        return pltpu.make_async_remote_copy(
            src_ref=part.at[s],
            dst_ref=rs.at[j],
            send_sem=e_send.at[E_RS, s],
            recv_sem=e_recv.at[E_RS, j],
            device_id={"tp": s},
            device_id_type=MESH,
        )

    def down(s):
        at = pl.ds(pl.multiple_of(s * rows(W_DOWN), 16), rows(W_DOWN))
        part[s] = jnp.dot(
            hidden[...], b_down[at, :], preferred_element_type=jnp.float32
        ).astype(jnp.bfloat16)
        pl.when(s != j)(lambda: rs_copy(s).start())

    own_copy(W_DOWN).wait()
    down(i)
    for d in range(1, n_fs):
        if d == n_fs - 1:
            serve_all(W_DOWN, d, down_half)

        def finish(s):
            wait_y(W_DOWN, s)
            down(s)

        each(d, finish)

    for o in range(1, n_tp):
        p = lax.rem(j + o, n_tp)
        pltpu.make_async_remote_copy(
            src_ref=part.at[p],
            dst_ref=rs.at[p],
            send_sem=e_send.at[E_RS, p],
            recv_sem=e_recv.at[E_RS, p],
            device_id={"tp": p},
            device_id_type=MESH,
        ).wait_recv()
    summed = part[j].astype(jnp.float32)
    for o in range(1, n_tp):
        summed = summed + rs[lax.rem(j + o, n_tp)].astype(jnp.float32)
    out[...] = (mixed[...] + summed).astype(jnp.bfloat16)

    for k in range(5):
        for q in range(SPLITS[k]):
            pl.when(has_right)(lambda k=k, q=q: z_copy(k, q, i, True, True).wait_send())
            pl.when(has_left)(lambda k=k, q=q: z_copy(k, q, i, False, True).wait_send())
            for d in range(1, n_fs):

                @pl.when(i - d >= 0)
                def _(k=k, q=q, d=d):
                    pl.when(has_right)(lambda: z_copy(k, q, i - d, True, False).wait_send())
                    y_copy(k, q, i - d, g).wait_send()

                @pl.when(i + d < n_fs)
                def _(k=k, q=q, d=d):
                    pl.when(has_left)(lambda: z_copy(k, q, i + d, False, False).wait_send())
                    y_copy(k, q, i + d, g).wait_send()

    for o in range(1, n_tp):
        e_copy(E_TOK, o, tokens, tok_at).wait_send()
        e_copy(E_GAIN, o, gain1, gain_at).wait_send()
        e_copy(E_POOL, o, own_pool, pool_at).wait_send()
        e_copy(E_SQ, o, own_sq, sq_at).wait_send()
        e_copy(E_X2, o, own_x2, x2_at).wait_send()
        rs_copy(lax.rem(j + o, n_tp)).wait_send()


def fused(
    n_fs,
    n_tp,
    tokens,
    norm_gain,
    in_weight,
    pool_weight,
    pool_scale,
    out_weight,
    ffn_gain,
    gate_weight,
    up_weight,
    down_weight,
):
    _, length, feat = tokens.shape
    channels, units = in_weight.shape[1], gate_weight.shape[1]
    weights = (in_weight, out_weight, gate_weight, up_weight, down_weight)
    wide = lambda v: jnp.broadcast_to(v, (8, v.shape[0]))
    vmem = pl.BlockSpec(memory_space=pltpu.VMEM)
    hbm = pl.BlockSpec(memory_space=pl.ANY)
    items = sum(SPLITS)
    bf16, f32 = jnp.bfloat16, jnp.float32
    sems = pltpu.SemaphoreType.DMA
    return pl.pallas_call(
        functools.partial(kernel, n_fs, n_tp),
        out_shape=jax.ShapeDtypeStruct((length, feat), bf16),
        in_specs=[vmem] * 5 + [hbm] * 5,
        out_specs=vmem,
        scratch_shapes=[pltpu.VMEM((n_fs * w.shape[0], w.shape[1]), bf16) for w in weights]
        + [
            pltpu.VMEM((length, n_tp * feat), bf16),
            pltpu.VMEM((8, n_tp * feat), f32),
            pltpu.VMEM((length, n_tp * channels), bf16),
            pltpu.VMEM((n_tp + 1, length, 128), f32),
            pltpu.VMEM((length, n_tp * feat), bf16),
            pltpu.VMEM((length, feat), f32),
            pltpu.VMEM((length, units), f32),
            pltpu.VMEM((length, units), bf16),
            pltpu.VMEM((n_tp, length, feat), bf16),
            pltpu.VMEM((n_tp, length, feat), bf16),
            pltpu.VMEM((length, channels + feat), bf16),
        ]
        + [sems((items, n_fs))] * 5
        + [sems((5,)), sems((6, n_tp)), sems((6, n_tp))],
        compiler_params=pltpu.CompilerParams(
            collective_id=0, has_side_effects=True, vmem_limit_bytes=56 * 1024 * 1024
        ),
    )(
        tokens[0],
        wide(norm_gain),
        pool_weight,
        wide(pool_scale),
        wide(ffn_gain),
        *weights,
    )[None]


def solution(mesh):
    n_grp, n_fs, n_tp = mesh.shape["grp"], mesh.shape["fs"], mesh.shape["tp"]
    body = functools.partial(fused, n_fs, n_tp) if n_grp == 2 and 4 <= n_fs == n_tp <= 8 else local
    return jax.shard_map(
        body,
        mesh=mesh,
        in_specs=(
            P(("grp", "fs"), None, "tp"),
            P("tp"),
            P("fs", "tp"),
            P("tp", None, None),
            P("tp"),
            P("fs", "tp"),
            P("tp"),
            P("fs", "tp"),
            P("fs", "tp"),
            P("tp", "fs"),
        ),
        out_specs=P(("grp", "fs"), None, "tp"),
        check_vma=False,
    )
```
